32 devices in a mesh: ep: 8 (over z, x), tp: 4 (over y, core).
Axes of the slice: x: 2, y: 2, z: 4, core: 2. Of those that a mesh axis runs over, the one named last changes fastest.
Arguments:
- mix_values: bfloat16 [4096, 2048], P('ep', 'tp'), may hold values from -6 to 6
- mix_inner_gate: bfloat16 [4096, 2048], P('ep', 'tp'), may hold values from -6 to 6
- mix_outer_gate: bfloat16 [4096, 2048], P('ep', 'tp'), may hold values from -6 to 6
- conv_taps: bfloat16 [3, 2048], replicated, may hold values from -3 to 3
- mix_out_weight: bfloat16 [2048, 2048], P('tp'), may hold values from -0.125 to 0.125
- moe_input: bfloat16 [4096, 2048], P('ep'), may hold values from -36 to 36
- norm_gain: float32 [2048], replicated, may hold values from 0.1 to 1.9
- routes: int32 [4096, 2], P('ep'), may hold values from 0 to 7, all different within a row; in each aligned block of 128 rows (0 to 127, 128 to 255, ...) at most 64 rows name the same one
- route_weights: float32 [4096, 2], P('ep'), may hold values from 0.05 to 1
- expert_gate: bfloat16 [8, 2048, 1024], P('ep', None, 'tp'), may hold values from -0.125 to 0.125
- expert_up: bfloat16 [8, 2048, 1024], P('ep', None, 'tp'), may hold values from -0.125 to 0.125
- expert_down: bfloat16 [8, 1024, 2048], P('ep', 'tp'), may hold values from -0.1875 to 0.1875
- shared_gate: bfloat16 [2048, 1024], P(None, 'tp'), may hold values from -0.125 to 0.125
- shared_up: bfloat16 [2048, 1024], P(None, 'tp'), may hold values from -0.125 to 0.125
- shared_down: bfloat16 [1024, 2048], P('tp'), may hold values from -0.1875 to 0.1875
Outputs:
- mixed_out: bfloat16 [4096, 2048], P(('ep', 'tp'))
- expert_out: bfloat16 [4096, 2048], P(('ep', 'tp'))
The draws below stay inside these ranges and needn't reach their ends.
Inputs may be any that keep to these rules, and one draw needn't show every extreme that they name: `routes`: each row names 2 different experts; in each aligned block of 128 rows no expert is named more than 64 times, and in every draw some block names some expert exactly 64 times.
All inputs are finite; a program needn't handle non-finite values.
Results may differ from the reference program's by a relative error of at most 0.012.
Values may be sent and summed in bfloat16 or wider, within the bound.
A program may use at most 128 MiB of HBM per device.

```python
import math
import jax
import jax.numpy as jnp
import numpy as np
from jax import lax

D = 2048
HID = 1024
TAPS = 3
TOP = 2
EXPERTS = 8
TOKENS_A = 4096
TOK_B = 128
TOKENS_B = 4096
CAP = 64
N_TP = 4


def draw_moe_input(key, part):
    base_key, row_key, column_key = jax.random.split(jax.random.fold_in(key, 17), 3)
    row_scale = 0.3 * jnp.exp(jax.random.uniform(row_key, (TOKENS_B, 1), jnp.float32, 0.0, math.log(10.0)))
    column_scale = 0.3 * jnp.exp(jax.random.uniform(column_key, (1, D), jnp.float32, 0.0, math.log(10.0)))
    base = jax.random.normal(base_key, (TOKENS_B, D), jnp.float32)
    return (jnp.clip(base, -4.0, 4.0) * row_scale * column_scale).astype(jnp.bfloat16)


def block_levels(key, shape, shards, smallest, top_value):
    def one(axis_at, shards_of):
        steps = jax.random.uniform(jax.random.fold_in(jax.random.fold_in(key, 6), axis_at), (shards_of,), jnp.float32, smallest / len(shards), top_value / len(shards))
        return jnp.repeat(jnp.exp(steps), shape[axis_at] // shards_of).reshape((-1,) + (1,) * (len(shape) - axis_at - 1))

    gain = one(*shards[0])
    for cut in shards[1:]:
        gain = gain * one(*cut)
    return gain


def assign_block(key, own, number, rows, number_of, top, reach, skew):
    order = jax.random.permutation(key, number_of)
    crowded, usual = shares(number_of, rows * top, reach, skew, True), shares(number_of, rows * top, reach, skew, False)
    places = jnp.arange(number_of)

    def named(tallies, turn):
        used = int((tallies > 0).sum())
        fixed = max(1, used // 4)
        shifted = fixed + (places - fixed + turn * (used - fixed)) % max(1, number_of - fixed)
        return jnp.zeros((number_of,), jnp.int32).at[order[jnp.where(places < fixed, places, shifted)]].set(jnp.asarray(tallies, jnp.int32))

    tallies = jnp.where(number % 4 == 0, named(crowded, number // 4), named(usual, number - number // 4 - 1))
    mixed = jax.random.permutation(jax.random.fold_in(own, 3), number_of)
    giver, taker = mixed[0:number_of // 2 * 2:2], mixed[1:number_of // 2 * 2:2]
    room = jnp.minimum(tallies[giver] - 1, reach - tallies[taker]) // 2
    room = jnp.where((giver == order[0]) | (taker == order[0]) | (tallies[taker] == 0), 0, jnp.maximum(room, 0))
    shifted = jax.random.randint(jax.random.fold_in(own, 4), (number_of // 2,), 0, 1 << 20) % (room + 1)
    tallies = tallies.at[giver].add(-shifted).at[taker].add(shifted)
    members = jnp.searchsorted(jnp.cumsum(tallies), jnp.arange(rows * top), side="right").astype(jnp.int32)
    table = members.reshape(top, rows).T
    table = table[jax.random.permutation(jax.random.fold_in(own, 1), rows)]
    turn = jax.random.randint(jax.random.fold_in(own, 2), (rows, 1), 0, top)
    return jnp.take_along_axis(table, (jnp.arange(top)[None, :] + turn) % top, axis=1)


def shares(count, total, most, slope, full):
    weights = [(1 << 20) // math.isqrt(rank ** slope) + 1 for rank in range(1, count + 1)]
    largest = most if full else min(most, max(-(-total // count), total * weights[0] // sum(weights)))
    least = 1 if total - largest >= count - 1 else 0
    holding, rest = [largest] + [least] * (count - 1), total - largest - least * (count - 1)
    while rest > 0:
        free = [i for i in range(1, count) if holding[i] < largest] or [i for i in range(1, count) if holding[i] < most]
        whole, remaining = sum([weights[i] for i in free]), rest
        for i in free:
            more = min(most - holding[i], max(1, remaining * weights[i] // whole), rest)
            holding[i] = holding[i] + more
            rest = rest - more
    return np.array(holding)


def gaussian(rng, extent, width, reach, cuts=(), kind=jnp.bfloat16):
    factor_of = block_levels(rng, extent, cuts, -0.22, 0.18) if cuts else 1.0
    drawn = jax.random.normal(rng, extent, jnp.float32) * width * factor_of
    return jnp.minimum(jnp.maximum(drawn, -reach), reach).astype(kind)


def setup_inputs(seed: int = 0) -> dict:
    key_list = jax.random.split(jax.random.key(seed), 16)
    mix_values = gaussian(key_list[0], (TOKENS_A, D), 1.0, 6.0, ((0, 8), (1, 4)))
    mix_inner_gate = gaussian(key_list[1], (TOKENS_A, D), 1.0, 6.0, ((0, 8), (1, 4)))
    mix_outer_gate = gaussian(key_list[2], (TOKENS_A, D), 1.0, 6.0, ((0, 8), (1, 4)))
    conv_taps = gaussian(key_list[3], (TAPS, D), 0.6, 3.0)
    mix_out_weight = gaussian(key_list[4], (D, D), D ** -0.5, 0.125, ((0, 4),))
    moe_input = draw_moe_input(jax.random.fold_in(key_list[15], 71), 0)
    norm_gain = jnp.clip(1.0 + 0.18 * jax.random.normal(key_list[6], (D,), jnp.float32), 0.1, 1.9)
    routes_keys = jax.random.split(jax.random.fold_in(key_list[7], 1), TOKENS_B // TOK_B)
    routes_turns = jax.random.permutation(jax.random.fold_in(key_list[7], 3), TOKENS_B // TOK_B)
    routes = jax.vmap(lambda own, number: assign_block(jax.random.fold_in(key_list[7], 2), own, number, TOK_B, EXPERTS, TOP, CAP, 2))(routes_keys, routes_turns).reshape((TOKENS_B, TOP))
    route_weights = jnp.clip(jnp.exp(math.log(1.0) - 2.9957323 * jax.random.uniform(key_list[8], (TOKENS_B, TOP), jnp.float32) ** block_levels(key_list[8], (TOKENS_B, TOP), ((0, 8),), -0.2, 0.2)), 0.05, 1.0)
    expert_gate = gaussian(key_list[9], (EXPERTS, D, HID), D ** -0.5, 0.125, ((0, 8), (2, 4)))
    expert_up = gaussian(key_list[10], (EXPERTS, D, HID), D ** -0.5, 0.125, ((0, 8), (2, 4)))
    expert_down = gaussian(key_list[11], (EXPERTS, HID, D), HID ** -0.5, 0.1875, ((0, 8), (1, 4)))
    shared_gate = gaussian(key_list[12], (D, HID), D ** -0.5, 0.125, ((1, 4),))
    shared_up = gaussian(key_list[13], (D, HID), D ** -0.5, 0.125, ((1, 4),))
    shared_down = gaussian(key_list[14], (HID, D), HID ** -0.5, 0.1875, ((0, 4),))
    return dict(mix_values=mix_values, mix_inner_gate=mix_inner_gate, mix_outer_gate=mix_outer_gate, conv_taps=conv_taps, mix_out_weight=mix_out_weight, moe_input=moe_input, norm_gain=norm_gain, routes=routes, route_weights=route_weights, expert_gate=expert_gate, expert_up=expert_up, expert_down=expert_down, shared_gate=shared_gate, shared_up=shared_up, shared_down=shared_down)


def dot_wide(left, right):
    return jnp.dot(left.astype(jnp.float32), right.astype(jnp.float32), preferred_element_type=jnp.float32)

def slot_table(route_block, experts, capacity):
    tokens, top = route_block.shape
    flat = route_block.reshape(-1).astype(jnp.int32)
    onehot = (flat[:, None] == jnp.arange(experts, dtype=jnp.int32)[None, :]).astype(jnp.int32)
    before = jnp.cumsum(onehot, axis=0) - onehot
    target = flat * capacity + lax.optimization_barrier(jnp.sum(before * onehot, axis=1))
    match = target[None, :] == jnp.arange(experts * capacity, dtype=jnp.int32)[:, None]
    owner = lax.optimization_barrier(jnp.sum(jnp.where(match, jnp.arange(tokens * top, dtype=jnp.int32)[None, :], 0), axis=1))
    filled = jnp.any(match, axis=1)
    return (target.reshape(tokens, top), owner.reshape(experts, capacity), filled.reshape(experts, capacity))

def rounded(values):
    return lax.optimization_barrier(values.astype(jnp.bfloat16)).astype(jnp.float32)

def reference(mix_values, mix_inner_gate, mix_outer_gate, conv_taps, mix_out_weight, moe_input, norm_gain, routes, route_weights, expert_gate, expert_up, expert_down, shared_gate, shared_up, shared_down):
    product = mix_inner_gate.astype(jnp.float32) * mix_values.astype(jnp.float32)
    length = product.shape[0]
    padded = jnp.concatenate([jnp.zeros((TAPS - 1, D), jnp.float32), product], axis=0)
    taps = conv_taps.astype(jnp.float32)
    convolved = taps[0] * padded[0:length]
    for offset in range(1, TAPS):
        convolved = convolved + taps[offset] * padded[offset:offset + length]
    gated_rows = (mix_outer_gate.astype(jnp.float32) * convolved).astype(jnp.bfloat16)
    mixed_out = dot_wide(gated_rows, mix_out_weight).astype(jnp.bfloat16)
    values = moe_input.astype(jnp.float32)
    scale = lax.rsqrt(lax.optimization_barrier(jnp.mean(values * values, axis=1, keepdims=True)) + 1e-06)
    normed = (values * scale * norm_gain).astype(jnp.bfloat16)
    part = HID // N_TP
    shared_hidden = (jax.nn.silu(dot_wide(normed, shared_gate)) * dot_wide(normed, shared_up)).astype(jnp.bfloat16)
    shared = jnp.zeros((normed.shape[0], D), jnp.float32)
    for quarter in range(N_TP):
        shared = shared + rounded(dot_wide(shared_hidden[:, quarter * part:(quarter + 1) * part], shared_down[quarter * part:(quarter + 1) * part]))
    blocks = normed.shape[0] // TOK_B
    unused, owners, filled = jax.vmap(lambda block: slot_table(block, EXPERTS, CAP))(routes.reshape(blocks, TOK_B, TOP))
    owners = owners + (jnp.arange(blocks, dtype=jnp.int32) * (TOK_B * TOP))[:, None, None]
    pairs_by_expert = owners.transpose(1, 0, 2).reshape(EXPERTS, blocks * CAP)
    valid_by_expert = filled.transpose(1, 0, 2).reshape(EXPERTS, blocks * CAP)
    mix_weights = 2.5 * route_weights / lax.optimization_barrier(jnp.sum(route_weights, axis=1, keepdims=True))
    flat_weights = mix_weights.reshape(-1)

    def per_expert(total, inputs):
        weight_gate, weight_up, weight_down, pairs, valid = inputs
        token_index = pairs // TOP
        rows = normed[token_index]
        hidden = (jax.nn.silu(dot_wide(rows, weight_gate)) * dot_wide(rows, weight_up)).astype(jnp.bfloat16)
        result = jnp.zeros((rows.shape[0], D), jnp.float32)
        for quarter in range(N_TP):
            result = result + rounded(dot_wide(hidden[:, quarter * part:(quarter + 1) * part], weight_down[quarter * part:(quarter + 1) * part]))
        result = rounded(result)
        share = jnp.where(valid, flat_weights[pairs], 0.0)
        return (total.at[token_index].add(result * share[:, None]), None)
    total, unused_out = lax.scan(per_expert, shared, (expert_gate, expert_up, expert_down, pairs_by_expert, valid_by_expert))
    return (mixed_out, total.astype(jnp.bfloat16))
```

```python
import jax
import jax.numpy as jnp
from jax import lax
from jax.sharding import PartitionSpec as P


def from_behind(value, axis, steps):
    count = lax.axis_size(axis)
    initial, last = (max(0, -steps), min(count, count - steps))
    return lax.ppermute(value, axis, [(source, source + steps) for source in range(initial, last)])


def normalized(rows, gain):
    values = rows.astype(jnp.float32)
    scale = lax.rsqrt(jnp.mean(values * values, axis=1, keepdims=True) + 1e-06)
    return (values * scale * gain).astype(jnp.bfloat16)


def slot_targets(route_block, experts, capacity):
    tokens, top = route_block.shape
    names = jnp.arange(experts, dtype=jnp.int32)[None, :]
    named = [route_block[:, k : k + 1] == names for k in range(top)]
    any_named = named[0]
    for k in range(1, top):
        any_named = any_named | named[k]
    earlier = (
        jnp.arange(tokens, dtype=jnp.int32)[:, None] > jnp.arange(tokens, dtype=jnp.int32)[None, :]
    )
    before = jnp.dot(
        earlier.astype(jnp.bfloat16),
        any_named.astype(jnp.bfloat16),
        preferred_element_type=jnp.float32,
    ).astype(jnp.int32)
    return [
        route_block[:, k : k + 1] * capacity
        + jnp.sum(jnp.where(named[k], before, 0), axis=1, keepdims=True)
        for k in range(top)
    ]


def on_device(
    mix_values,
    mix_inner_gate,
    mix_outer_gate,
    conv_taps,
    mix_out_weight,
    moe_input,
    norm_gain,
    routes,
    route_weights,
    expert_gate,
    expert_up,
    expert_down,
    shared_gate,
    shared_up,
    shared_down,
):
    parts = lax.axis_size("tp")
    member = lax.axis_index("tp")
    groups = lax.axis_size("ep")
    rows_here, width_here = mix_values.shape
    reach = conv_taps.shape[0] - 1
    taps = lax.dynamic_slice_in_dim(conv_taps, member * width_here, width_here, 1).astype(
        jnp.float32
    )
    boundary = from_behind(
        jnp.stack([mix_values[rows_here - reach :], mix_inner_gate[rows_here - reach :]]), "ep", 1
    )
    product = jnp.concatenate(
        [
            boundary[1].astype(jnp.float32) * boundary[0].astype(jnp.float32),
            mix_inner_gate.astype(jnp.float32) * mix_values.astype(jnp.float32),
        ],
        axis=0,
    )
    convolved = taps[0] * product[0:rows_here]
    for offset in range(1, reach + 1):
        convolved = convolved + taps[offset] * product[offset : offset + rows_here]
    gated_rows = (mix_outer_gate.astype(jnp.float32) * convolved).astype(jnp.bfloat16)
    mixed = lax.psum_scatter(
        jnp.dot(gated_rows, mix_out_weight, preferred_element_type=jnp.float32).astype(
            jnp.bfloat16
        ),
        "tp",
        scatter_dimension=0,
        tiled=True,
    )
    local_experts = expert_gate.shape[0]
    experts = local_experts * groups
    width = moe_input.shape[1]
    block = moe_input.shape[0] // parts
    top = routes.shape[1]
    capacity = 2 * block * top // experts
    whole_gate = lax.all_gather(expert_gate, "tp", axis=0)
    whole_up = lax.all_gather(expert_up, "tp", axis=0)
    whole_down = lax.all_gather(expert_down, "tp", axis=0)

    own_rows = normalized(
        lax.dynamic_slice_in_dim(moe_input, member * block, block, 0), norm_gain
    )
    own_routes = lax.dynamic_slice_in_dim(routes, member * block, block, 0)
    targets = slot_targets(own_routes, experts, capacity)
    slots = jnp.arange(experts * capacity, dtype=jnp.int32)[None, :]
    picks = [(target == slots).astype(jnp.bfloat16) for target in targets]
    placed = picks[0]
    for k in range(1, top):
        placed = placed + picks[k]
    sent = lax.dot_general(
        placed, own_rows, (((0,), (0,)), ((), ())), preferred_element_type=jnp.float32
    ).astype(jnp.bfloat16)
    arrived = lax.all_to_all(
        sent.reshape(groups, local_experts * capacity, width),
        "ep",
        split_axis=0,
        concat_axis=0,
        tiled=True,
    ).reshape(groups, local_experts, capacity, width)

    normed_all = normalized(moe_input, norm_gain)
    shared_gate_part = jnp.dot(normed_all, shared_gate, preferred_element_type=jnp.float32)
    shared_up_part = jnp.dot(normed_all, shared_up, preferred_element_type=jnp.float32)
    hidden_shared = (jax.nn.silu(shared_gate_part) * shared_up_part).astype(jnp.bfloat16)
    shared = lax.psum_scatter(
        jnp.dot(hidden_shared, shared_down, preferred_element_type=jnp.float32).astype(
            jnp.bfloat16
        ),
        "tp",
        scatter_dimension=0,
        tiled=True,
    ).astype(jnp.float32)

    finished = []
    for expert in range(local_experts):
        rows = arrived[:, expert].reshape(groups * capacity, width)
        hidden = []
        for part in range(parts):
            gate_part = jnp.dot(
                rows, whole_gate[part, expert], preferred_element_type=jnp.float32
            )
            up_part = jnp.dot(rows, whole_up[part, expert], preferred_element_type=jnp.float32)
            hidden.append((jax.nn.silu(gate_part) * up_part).astype(jnp.bfloat16))
        down = whole_down[:, expert].reshape(-1, width)
        finished.append(
            jnp.dot(
                jnp.concatenate(hidden, axis=1), down, preferred_element_type=jnp.float32
            )
            .astype(jnp.bfloat16)
            .reshape(groups, 1, capacity, width)
        )
    routed_back = finished[0] if local_experts == 1 else jnp.concatenate(finished, axis=1)
    returned = lax.all_to_all(
        routed_back.reshape(groups, local_experts * capacity, width),
        "ep",
        split_axis=0,
        concat_axis=0,
        tiled=True,
    ).reshape(experts * capacity, width)
    own_weights = lax.dynamic_slice_in_dim(route_weights, member * block, block, 0)
    mix_weights = 2.5 * own_weights / jnp.sum(own_weights, axis=1, keepdims=True)
    total = shared
    for k in range(top):
        chosen = jnp.dot(picks[k], returned, preferred_element_type=jnp.float32)
        total = total + mix_weights[:, k : k + 1] * chosen
    expert_out = total.astype(jnp.bfloat16)
    return (mixed, expert_out)


def solution(mesh):
    return jax.shard_map(
        on_device,
        mesh=mesh,
        in_specs=(
            P("ep", "tp"),
            P("ep", "tp"),
            P("ep", "tp"),
            P(),
            P("tp", None),
            P("ep", None),
            P(),
            P("ep", None),
            P("ep", None),
            P("ep", None, "tp"),
            P("ep", None, "tp"),
            P("ep", "tp", None),
            P(None, "tp"),
            P(None, "tp"),
            P("tp", None),
        ),
        out_specs=(P(("ep", "tp"), None), P(("ep", "tp"), None)),
        check_vma=False,
    )
```

```python
import jax
import jax.numpy as jnp
from jax import lax
from jax.sharding import PartitionSpec as P


def from_behind(value, axis, steps):
    count = lax.axis_size(axis)
    initial, last = (max(0, -steps), min(count, count - steps))
    return lax.ppermute(value, axis, [(source, source + steps) for source in range(initial, last)])


def across(value, axis, stride):
    count = lax.axis_size(axis)
    return lax.ppermute(value, axis, [(source, source ^ stride) for source in range(count)])


def gathered_parts(shard, axis):
    count = lax.axis_size(axis)
    if count & (count - 1):
        whole = lax.all_gather(shard, axis, axis=0)
        return [whole[part] for part in range(count)]
    held = [shard]
    stride = count // 2
    while stride:
        held = [piece for value in held for piece in (value, across(value, axis, stride))]
        stride //= 2
    return held


def scattered_sum(rows, axis):
    count = lax.axis_size(axis)
    if count & (count - 1):
        return lax.psum_scatter(rows, axis, scatter_dimension=0, tiled=True).astype(jnp.float32)
    here = lax.axis_index(axis)
    block = rows.shape[0] // count
    held = rows.reshape((count, block) + rows.shape[1:])
    stride = 1
    while stride < count:
        bit = (here // stride) % 2
        pairs = held.reshape((held.shape[0] // 2, 2) + held.shape[1:])
        kept = lax.dynamic_index_in_dim(pairs, bit, 1, keepdims=False)
        given = lax.dynamic_index_in_dim(pairs, 1 - bit, 1, keepdims=False)
        got = across(given.astype(jnp.bfloat16), axis, stride)
        held = kept.astype(jnp.float32) + got.astype(jnp.float32)
        stride *= 2
    return held.reshape((block,) + rows.shape[1:]).astype(jnp.float32)


def normalized(rows, gain):
    values = rows.astype(jnp.float32)
    scale = lax.rsqrt(jnp.mean(values * values, axis=1, keepdims=True) + 1e-06)
    return (values * scale * gain).astype(jnp.bfloat16)


def slot_targets(route_block, experts, capacity):
    tokens, top = route_block.shape
    names = jnp.arange(experts, dtype=jnp.int32)[None, :]
    named = [route_block[:, k : k + 1] == names for k in range(top)]
    any_named = named[0]
    for k in range(1, top):
        any_named = any_named | named[k]
    earlier = (
        jnp.arange(tokens, dtype=jnp.int32)[:, None] > jnp.arange(tokens, dtype=jnp.int32)[None, :]
    )
    before = jnp.dot(
        earlier.astype(jnp.bfloat16),
        any_named.astype(jnp.bfloat16),
        preferred_element_type=jnp.float32,
    ).astype(jnp.int32)
    return [
        route_block[:, k : k + 1] * capacity
        + jnp.sum(jnp.where(named[k], before, 0), axis=1, keepdims=True)
        for k in range(top)
    ]


def on_device(
    mix_values,
    mix_inner_gate,
    mix_outer_gate,
    conv_taps,
    mix_out_weight,
    moe_input,
    norm_gain,
    routes,
    route_weights,
    expert_gate,
    expert_up,
    expert_down,
    shared_gate,
    shared_up,
    shared_down,
):
    parts = lax.axis_size("tp")
    member = lax.axis_index("tp")
    groups = lax.axis_size("ep")
    rows_here, width_here = mix_values.shape
    reach = conv_taps.shape[0] - 1
    taps = lax.dynamic_slice_in_dim(conv_taps, member * width_here, width_here, 1).astype(
        jnp.float32
    )
    boundary = from_behind(
        jnp.stack([mix_values[rows_here - reach :], mix_inner_gate[rows_here - reach :]]), "ep", 1
    )
    local_experts = expert_gate.shape[0]
    experts = local_experts * groups
    width = moe_input.shape[1]
    block = moe_input.shape[0] // parts
    top = routes.shape[1]
    capacity = 2 * block * top // experts
    gate_parts = gathered_parts(expert_gate, "tp")
    up_parts = gathered_parts(expert_up, "tp")
    down_parts = gathered_parts(expert_down, "tp")
    whole_gate = lax.optimization_barrier(jnp.concatenate(gate_parts, axis=2))
    whole_up = lax.optimization_barrier(jnp.concatenate(up_parts, axis=2))

    own_rows = normalized(
        lax.dynamic_slice_in_dim(moe_input, member * block, block, 0), norm_gain
    )
    own_routes = lax.dynamic_slice_in_dim(routes, member * block, block, 0)
    targets = slot_targets(own_routes, experts, capacity)
    slots = jnp.arange(experts * capacity, dtype=jnp.int32)[None, :]
    picks = [(target == slots).astype(jnp.bfloat16) for target in targets]
    placed = picks[0]
    for k in range(1, top):
        placed = placed + picks[k]
    sent = lax.dot_general(
        placed, own_rows, (((0,), (0,)), ((), ())), preferred_element_type=jnp.float32
    ).astype(jnp.bfloat16)
    sent, boundary = lax.optimization_barrier((sent, boundary))
    arrived = lax.all_to_all(
        sent.reshape(groups, local_experts * capacity, width),
        "ep",
        split_axis=0,
        concat_axis=0,
        tiled=True,
    ).reshape(groups, local_experts, capacity, width)

    product = jnp.concatenate(
        [
            boundary[1].astype(jnp.float32) * boundary[0].astype(jnp.float32),
            mix_inner_gate.astype(jnp.float32) * mix_values.astype(jnp.float32),
        ],
        axis=0,
    )
    convolved = taps[0] * product[0:rows_here]
    for offset in range(1, reach + 1):
        convolved = convolved + taps[offset] * product[offset : offset + rows_here]
    gated_rows = (mix_outer_gate.astype(jnp.float32) * convolved).astype(jnp.bfloat16)
    mixed_part = jnp.dot(
        gated_rows, mix_out_weight, preferred_element_type=jnp.float32
    ).astype(jnp.bfloat16)
    mixed = scattered_sum(mixed_part, "tp").astype(jnp.bfloat16)

    normed_all = normalized(moe_input, norm_gain)
    shared_gate_part = jnp.dot(normed_all, shared_gate, preferred_element_type=jnp.float32)
    shared_up_part = jnp.dot(normed_all, shared_up, preferred_element_type=jnp.float32)
    hidden_shared = (jax.nn.silu(shared_gate_part) * shared_up_part).astype(jnp.bfloat16)
    shared_part = jnp.dot(
        hidden_shared, shared_down, preferred_element_type=jnp.float32
    ).astype(jnp.bfloat16)
    shared = scattered_sum(shared_part, "tp")

    finished = []
    for expert in range(local_experts):
        rows = arrived[:, expert].reshape(groups * capacity, width)
        gate_part = jnp.dot(rows, whole_gate[expert], preferred_element_type=jnp.float32)
        up_part = jnp.dot(rows, whole_up[expert], preferred_element_type=jnp.float32)
        hidden = (jax.nn.silu(gate_part) * up_part).astype(jnp.bfloat16)
        part_width = hidden.shape[1] // parts
        result = jnp.zeros((), jnp.float32)
        span = max(1, parts // 2)
        for start in range(0, parts, span):
            result = result + jnp.dot(
                hidden[:, start * part_width : (start + span) * part_width],
                jnp.concatenate(
                    [piece[expert] for piece in down_parts[start : start + span]], axis=0
                ),
                preferred_element_type=jnp.float32,
            )
        finished.append(result.astype(jnp.bfloat16).reshape(groups, 1, capacity, width))
    routed_back = finished[0] if local_experts == 1 else jnp.concatenate(finished, axis=1)
    returned = lax.all_to_all(
        routed_back.reshape(groups, local_experts * capacity, width),
        "ep",
        split_axis=0,
        concat_axis=0,
        tiled=True,
    ).reshape(experts * capacity, width)
    own_weights = lax.dynamic_slice_in_dim(route_weights, member * block, block, 0)
    mix_weights = 2.5 * own_weights / jnp.sum(own_weights, axis=1, keepdims=True)
    total = shared
    for k in range(top):
        chosen = jnp.dot(picks[k], returned, preferred_element_type=jnp.float32)
        total = total + mix_weights[:, k : k + 1] * chosen
    expert_out = total.astype(jnp.bfloat16)
    return (mixed, expert_out)


def solution(mesh):
    return jax.shard_map(
        on_device,
        mesh=mesh,
        in_specs=(
            P("ep", "tp"),
            P("ep", "tp"),
            P("ep", "tp"),
            P(),
            P("tp", None),
            P("ep", None),
            P(),
            P("ep", None),
            P("ep", None),
            P("ep", None, "tp"),
            P("ep", None, "tp"),
            P("ep", "tp", None),
            P(None, "tp"),
            P(None, "tp"),
            P("tp", None),
        ),
        out_specs=(P(("ep", "tp"), None), P(("ep", "tp"), None)),
        check_vma=False,
    )
```
